32 devices in a mesh: ep: 8 (over z, y), tp: 4 (over x, core).
Axes of the slice: x: 2, y: 2, z: 4, core: 2. Of those that a mesh axis runs over, the one named last changes fastest.
Arguments:
- queries: bfloat16 [1536, 8, 128], P('ep', 'tp'), may hold values from -140 to 140
- keys: bfloat16 [1536, 4, 128], P('ep', 'tp'), may hold values from -6 to 6
- values: bfloat16 [1536, 4, 128], P('ep', 'tp'), may hold values from -6 to 6
- mix_scale: float32 [8], P('tp'), may hold values from 0.3 to 0.8
- head_gain: float32 [128], replicated, may hold values from 0.1 to 1.9
- out_weight: bfloat16 [8, 128, 2048], P('tp'), may hold values from -0.1875 to 0.1875
- moe_input: bfloat16 [3072, 2048], P(('ep', 'tp')), may hold values from -6 to 6
- norm_gain: float32 [2048], replicated, may hold values from 0.1 to 1.9
- routes: int32 [3072, 2], P(('ep', 'tp')), may hold values from 0 to 7, all different within a row; in each aligned block of 96 rows (0 to 95, 96 to 191, ...) at most 36 rows name the same one
- route_weights: float32 [3072, 2], P(('ep', 'tp')), may hold values from 0.2 to 1
- gate_weight: bfloat16 [8, 2048, 3584], P('ep', None, 'tp'), may hold values from -0.125 to 0.125
- up_weight: bfloat16 [8, 2048, 3584], P('ep', None, 'tp'), may hold values from -0.125 to 0.125
- down_weight: bfloat16 [8, 3584, 2048], P('ep', 'tp'), may hold values from -0.09375 to 0.09375
Outputs:
- attn_out: bfloat16 [1536, 2048], P(('ep', 'tp'))
- moe_out: bfloat16 [3072, 2048], P(('ep', 'tp'))
The draws below stay inside these ranges and needn't reach their ends.
Inputs may be any that keep to these rules, and one draw needn't show every extreme that they name: `routes`: the 2 experts of a row differ. In each aligned block of 96 rows (the rows of one device) no expert is named by more than 36 rows, and in some blocks an expert is named by exactly 36 rows.
All inputs are finite; a program needn't handle non-finite values.
Results may differ from the reference program's by a relative error of at most 0.014.
Values may be sent and summed in bfloat16 or wider, within the bound.
No kernel may reach another device: no remote copies, remote signals or barrier semaphores. Data moves between devices by JAX's collectives and lax.ppermute only.
A program may use at most 128 MiB of HBM per device.

```python
import math
import jax
import jax.numpy as jnp
import numpy as np
from jax import lax

D = 2048
HEADS = 8
KV_HEADS = 4
HD = 64
VD = 128
FFE = 3584
TOPK = 2
TA = 192
TOK_M = 96
SEQ = 1536
TOKENS_M = 3072
EXPERTS = 8
CAP = 36
N_EP = 8
N_TP = 4


def plant_rows(key):
    base = jax.random.fold_in(key, 11)
    query_key, key_key = jax.random.split(base, 2)
    query_draw = 1.3 * jax.random.truncated_normal(query_key, -4.0, 4.0, (SEQ, HEADS, 2, HD), jnp.float32)
    key_draw = 1.3 * jax.random.truncated_normal(key_key, -4.0, 4.0, (SEQ, KV_HEADS, 2, HD), jnp.float32)
    return (query_draw.reshape(SEQ, HEADS, 2 * HD), key_draw.reshape(SEQ, KV_HEADS, 2 * HD))


def draw_queries(key, part):
    return plant_rows(key)[0].astype(jnp.bfloat16)


def draw_keys(key, part):
    return plant_rows(key)[1].astype(jnp.bfloat16)


def steps_of(rng, dims, cuts, smallest, high):
    level, own = 1.0, jax.random.fold_in(rng, 6)
    for position, shards_of in cuts:
        heights = jnp.exp(jax.random.uniform(jax.random.fold_in(own, position), (shards_of,), jnp.float32, smallest / len(cuts), high / len(cuts)))
        level = level * jnp.repeat(heights, dims[position] // shards_of).reshape([-1 if axis == position else 1 for axis in range(len(dims))])
    return level


def deal_out(stream_key, own, number, rows, count, top, most, lean):
    sequence = jax.random.permutation(stream_key, count)
    packed, common = portions_of(count, rows * top, most, lean, True), portions_of(count, rows * top, most, lean, False)
    places = jnp.arange(count)

    def named(sizes, turn):
        used = int((sizes > 0).sum())
        fixed = max(1, used // 4)
        shifted = fixed + (places - fixed + turn * (used - fixed)) % max(1, count - fixed)
        return jnp.zeros((count,), jnp.int32).at[sequence[jnp.where(places < fixed, places, shifted)]].set(jnp.asarray(sizes, jnp.int32))

    sizes = jnp.where(number % 4 == 0, named(packed, number // 4), named(common, number - number // 4 - 1))
    mixed = jax.random.permutation(jax.random.fold_in(own, 3), count)
    source_of, taker = mixed[0:count // 2 * 2:2], mixed[1:count // 2 * 2:2]
    margin = jnp.minimum(sizes[source_of] - 1, most - sizes[taker]) // 2
    margin = jnp.where((source_of == sequence[0]) | (taker == sequence[0]) | (sizes[taker] == 0), 0, jnp.maximum(margin, 0))
    shifted = jax.random.randint(jax.random.fold_in(own, 4), (count // 2,), 0, 1 << 20) % (margin + 1)
    sizes = sizes.at[source_of].add(-shifted).at[taker].add(shifted)
    items = jnp.searchsorted(jnp.cumsum(sizes), jnp.arange(rows * top), side="right").astype(jnp.int32)
    table = items.reshape(top, rows).T
    table = table[jax.random.permutation(jax.random.fold_in(own, 1), rows)]
    turn = jax.random.randint(jax.random.fold_in(own, 2), (rows, 1), 0, top)
    return jnp.take_along_axis(table, (jnp.arange(top)[None, :] + turn) % top, axis=1)


def portions_of(count, total, bound, lean, full):
    loads = [(1 << 20) // math.isqrt(grade ** lean) + 1 for grade in range(1, count + 1)]
    largest = bound if full else min(bound, max(-(-total // count), total * loads[0] // sum(loads)))
    least = 1 if total - largest >= count - 1 else 0
    counts, spare = [largest] + [least] * (count - 1), total - largest - least * (count - 1)
    while spare > 0:
        free = [i for i in range(1, count) if counts[i] < largest] or [i for i in range(1, count) if counts[i] < bound]
        mass, remaining = sum([loads[i] for i in free]), spare
        for i in free:
            more = min(bound - counts[i], max(1, remaining * loads[i] // mass), spare)
            counts[i] = counts[i] + more
            spare = spare - more
    return np.array(counts)


def normal_values(stream_key, extent, scale, reach, pieces=(), kind=jnp.bfloat16):
    entries = scale * jax.random.normal(stream_key, extent, jnp.float32)
    if pieces:
        entries = entries * steps_of(stream_key, extent, pieces, -0.22, 0.18)
    return jnp.clip(entries, -reach, reach).astype(kind)


def setup_inputs(seed: int = 0) -> dict:
    splits = jax.random.split(jax.random.key(seed), 14)
    queries = draw_queries(jax.random.fold_in(splits[13], 71), 0)
    keys = draw_keys(jax.random.fold_in(splits[13], 71), 0)
    values = normal_values(splits[2], (SEQ, KV_HEADS, VD), 1.0, 6.0, ((0, 8), (1, 4)))
    mix_scale = jnp.clip(0.3 + 0.5 * jax.random.uniform(splits[3], (HEADS,), jnp.float32) ** steps_of(splits[3], (HEADS,), ((0, 4),), -0.2, 0.2), 0.3, 0.8)
    head_gain = jnp.clip(1.0 + 0.18 * jax.random.normal(splits[4], (VD,), jnp.float32), 0.1, 1.9)
    out_weight = normal_values(splits[5], (HEADS, VD, D), (HEADS * VD) ** -0.5, 0.1875, ((0, 4),))
    moe_input = normal_values(splits[6], (TOKENS_M, D), 1.0, 6.0, ((0, 32),))
    norm_gain = jnp.clip(1.0 + 0.18 * jax.random.normal(splits[7], (D,), jnp.float32), 0.1, 1.9)
    routes_keys = jax.random.split(jax.random.fold_in(splits[8], 1), TOKENS_M // TOK_M)
    routes_turns = jax.random.permutation(jax.random.fold_in(splits[8], 3), TOKENS_M // TOK_M)
    routes = jax.vmap(lambda own, number: deal_out(jax.random.fold_in(splits[8], 2), own, number, TOK_M, EXPERTS, TOPK, CAP, 1))(routes_keys, routes_turns).reshape((TOKENS_M, TOPK))
    route_weights = jnp.clip(0.2 + 0.8 * jax.random.uniform(splits[9], (TOKENS_M, TOPK), jnp.float32) ** steps_of(splits[9], (TOKENS_M, TOPK), ((0, 32),), -0.2, 0.2), 0.2, 1.0)
    gate_weight = normal_values(splits[10], (EXPERTS, D, FFE), D ** -0.5, 0.125, ((0, 8), (2, 4)))
    up_weight = normal_values(splits[11], (EXPERTS, D, FFE), D ** -0.5, 0.125, ((0, 8), (2, 4)))
    down_weight = normal_values(splits[12], (EXPERTS, FFE, D), FFE ** -0.5, 0.09375, ((0, 8), (1, 4)))
    return dict(queries=queries, keys=keys, values=values, mix_scale=mix_scale, head_gain=head_gain, out_weight=out_weight, moe_input=moe_input, norm_gain=norm_gain, routes=routes, route_weights=route_weights, gate_weight=gate_weight, up_weight=up_weight, down_weight=down_weight)


def reference(queries, keys, values, mix_scale, head_gain, out_weight, moe_input, norm_gain, routes, route_weights, gate_weight, up_weight, down_weight):
    group_size = HEADS // KV_HEADS
    key_table = jnp.repeat(keys.reshape(SEQ, KV_HEADS, 2, HD), group_size, axis=1).astype(jnp.float32)
    value_table = jnp.repeat(values, group_size, axis=1).astype(jnp.float32)
    query_table = queries.reshape(SEQ, HEADS, 2, HD)
    key_positions = jnp.arange(SEQ, dtype=jnp.int32)

    def attend_block(block_id):
        first_row = block_id * TA
        query_block = lax.dynamic_slice_in_dim(query_table, first_row, TA, 0).astype(jnp.float32)
        scores = jnp.einsum('thmd,shmd->hmts', query_block, key_table) / math.sqrt(HD)
        positions = first_row + jnp.arange(TA, dtype=jnp.int32)
        visible = key_positions[None, :] <= positions[:, None]
        scores = jnp.where(visible, scores, -jnp.inf)
        row_peak = lax.optimization_barrier(jnp.max(scores, axis=-1, keepdims=True))
        weights = jnp.where(visible, jnp.exp(scores - row_peak), 0.0)
        totals = lax.optimization_barrier(jnp.sum(weights, axis=-1))
        rounded = lax.optimization_barrier(weights.astype(jnp.bfloat16)).astype(jnp.float32)
        numerator = jnp.einsum('hmts,shv->hmtv', rounded, value_table)
        blended = numerator[:, 0] / totals[:, 0, :, None] - mix_scale[:, None, None] * (numerator[:, 1] / totals[:, 1, :, None])
        normed = blended * lax.rsqrt(lax.optimization_barrier(jnp.mean(blended * blended, axis=-1, keepdims=True)) + 1e-05) * head_gain
        return jnp.transpose(normed.astype(jnp.bfloat16), (1, 0, 2))
    attended = lax.map(attend_block, jnp.arange(N_EP, dtype=jnp.int32)).reshape(SEQ, HEADS * VD)
    heads_group = HEADS // N_TP
    attn_sum = jnp.zeros((SEQ, D), jnp.float32)
    for member in range(N_TP):
        columns = attended[:, member * heads_group * VD:(member + 1) * heads_group * VD]
        weight_rows = out_weight[member * heads_group:(member + 1) * heads_group].reshape(heads_group * VD, D)
        head_part = jnp.dot(columns, weight_rows, preferred_element_type=jnp.float32).astype(jnp.bfloat16)
        attn_sum = attn_sum + head_part.astype(jnp.float32)
    attn_out = attn_sum.astype(jnp.bfloat16)
    widened = moe_input.astype(jnp.float32)
    normed_in = (widened * lax.rsqrt(lax.optimization_barrier(jnp.mean(widened * widened, axis=-1, keepdims=True)) + 1e-06) * norm_gain).astype(jnp.bfloat16)
    padded = jnp.concatenate([normed_in, jnp.zeros((1, D), jnp.bfloat16)], axis=0)
    limit = TOKENS_M // TOK_M * CAP
    width = FFE // N_TP

    def expert_step(running, expert_id):
        matches = routes == expert_id
        chosen = jnp.any(matches, axis=1)
        weight_row = lax.optimization_barrier(jnp.sum(jnp.where(matches, route_weights, 0.0), axis=1))
        row_ids = jnp.nonzero(chosen, size=limit, fill_value=TOKENS_M)[0].astype(jnp.int32)
        selected = padded[row_ids]
        gate_proj = jnp.dot(selected, gate_weight[expert_id], preferred_element_type=jnp.float32)
        up_proj = jnp.dot(selected, up_weight[expert_id], preferred_element_type=jnp.float32)
        hidden = (jax.nn.silu(gate_proj) * up_proj).astype(jnp.bfloat16)
        down_rows = down_weight[expert_id]
        summed = jnp.zeros((limit, D), jnp.float32)
        for member in range(N_TP):
            part = jnp.dot(hidden[:, member * width:(member + 1) * width], down_rows[member * width:(member + 1) * width], preferred_element_type=jnp.float32)
            summed = summed + part.astype(jnp.bfloat16).astype(jnp.float32)
        expert_out = summed.astype(jnp.bfloat16)
        row_weights = jnp.concatenate([weight_row, jnp.zeros((1,), jnp.float32)])[row_ids]
        running = running.at[row_ids].add(row_weights[:, None] * expert_out.astype(jnp.float32), mode='drop')
        return (running, None)
    collected, _ = lax.scan(expert_step, jnp.zeros((TOKENS_M, D), jnp.float32), jnp.arange(EXPERTS, dtype=jnp.int32))
    return (attn_out, collected.astype(jnp.bfloat16))
```

```python
import functools
import math

import jax
import jax.numpy as jnp
from jax import lax
from jax.experimental import pallas as pl
from jax.experimental.pallas import tpu as pltpu
from jax.sharding import PartitionSpec as P

NEG_LARGE = -1e30
VMEM_LIMIT = 24 * 1024 * 1024
EXPERT_VMEM = 24 * 1024 * 1024
SMALL_VMEM = 12 * 1024 * 1024


def swap(array, axis, bits):
    pairs = [(j, j ^ bits) for j in range(lax.axis_size(axis))]
    return lax.ppermute(array, axis, pairs)


def upward(array, axis, bit):
    pairs = [(j, j ^ bit) for j in range(lax.axis_size(axis)) if not j & bit]
    return lax.ppermute(array, axis, pairs)


def bits_of(axis):
    size = lax.axis_size(axis)
    return [1 << n for n in range(size.bit_length() - 1)]


def spread(piece, axis):
    bits = bits_of(axis)
    pieces = {0: piece}
    for bit in reversed(bits):
        for key in sorted(pieces):
            pieces[key | bit] = swap(pieces[key], axis, bit)
    return [pieces[key] for key in range(1 << len(bits))]


def total(terms):
    return sum(term.astype(jnp.float32) for term in terms).astype(jnp.bfloat16)


def gather_sum(keep, give, axis):
    bits = bits_of(axis)
    got = swap(give, axis, bits[0])
    parts = {2 * n: [keep[n], got[n]] for n in range(keep.shape[0])}
    for bit in bits[1:]:
        keys = [key for key in parts if not key & bit]
        if len(keys) == 1:
            sent = [swap(total(parts[key | bit]), axis, bit) for key in keys]
        else:
            sent = jnp.stack([total(parts[key | bit]) for key in keys])
            sent = swap(sent, axis, bit)
        parts = {key: parts[key] + [sent[n]] for n, key in enumerate(keys)}
    return [keep, got] + parts[0][2:]


def first_rows(terms):
    return [term[0] if term.ndim == 3 else term for term in terms]


def tokens_kernel(experts, base_ref, *refs):
    sources, outs = refs[:4], refs[4:-5]
    x_ref, gain_ref, routes_ref, shares_ref = refs[-5:-1]
    *blocks, mix_ref = outs
    loads = [
        pltpu.make_async_copy(source, target, refs[-1].at[n])
        for n, (source, target) in enumerate(zip(sources, refs[-5:-1]))
    ]
    for load in loads:
        load.start()
    for load in loads:
        load.wait()
    tok_count = x_ref.shape[0]
    rows = mix_ref.shape[2]
    wide = x_ref[...].astype(jnp.float32)
    normed = wide * lax.rsqrt(jnp.mean(wide * wide, axis=-1, keepdims=True) + 1e-06)
    normed = (normed * gain_ref[...]).astype(jnp.bfloat16)
    routes, shares = routes_ref[...], shares_ref[...]
    expert = lax.broadcasted_iota(jnp.int32, (experts, tok_count), 0) ^ base_ref[0]
    named = jnp.zeros((experts, tok_count), jnp.float32)
    share = jnp.zeros((experts, tok_count), jnp.float32)
    for k in range(routes.shape[0]):
        hit = routes[k : k + 1, :] == expert
        named = named + jnp.where(hit, 1.0, 0.0)
        share = share + jnp.where(hit, shares[k : k + 1, :], 0.0)
    row = lax.broadcasted_iota(jnp.int32, (tok_count, tok_count), 0)
    col = lax.broadcasted_iota(jnp.int32, (tok_count, tok_count), 1)
    earlier = jnp.where(row < col, 1.0, 0.0).astype(jnp.bfloat16)
    ranks = jnp.dot(named.astype(jnp.bfloat16), earlier, preferred_element_type=jnp.float32)
    places = jnp.where(named > 0.5, ranks, -1.0)
    slot = lax.broadcasted_iota(jnp.int32, (rows, tok_count), 0).astype(jnp.float32)
    picks = [jnp.where(places[k : k + 1, :] == slot, 1.0, 0.0) for k in range(experts)]
    pick = jnp.concatenate(picks, axis=0).astype(jnp.bfloat16)
    sent = jnp.dot(pick, normed, preferred_element_type=jnp.float32).astype(jnp.bfloat16)
    if len(blocks) == 1:
        blocks[0][...] = sent
    else:
        half = sent.shape[1] // 2
        for k in range(experts):
            for side in range(2):
                part = sent[k * rows : (k + 1) * rows, side * half : (side + 1) * half]
                blocks[k][side * rows : (side + 1) * rows, :] = part
    for k in range(experts):
        mix = picks[k] * share[k : k + 1, :]
        high = mix.astype(jnp.bfloat16)
        mix_ref[0, k] = high
        mix_ref[1, k] = (mix - high.astype(jnp.float32)).astype(jnp.bfloat16)


def route_tokens(base, moe_input, norm_gain, routes, route_weights, experts, capacity, split):
    tok_count, width = moe_input.shape
    operands = [moe_input, norm_gain.reshape(1, -1), routes.T, route_weights.T]
    operands = [pltpu.with_memory_space_constraint(a, pltpu.HBM) for a in operands]
    unit = 4 if split else 8
    rows = -(-capacity // unit) * unit
    if split:
        shapes = [jax.ShapeDtypeStruct((2 * rows, width // 2), jnp.bfloat16)] * experts
    else:
        shapes = [jax.ShapeDtypeStruct((experts * rows, width), jnp.bfloat16)]
    shapes.append(jax.ShapeDtypeStruct((2, experts, rows, tok_count), jnp.bfloat16))
    return pl.pallas_call(
        lambda *refs: tokens_kernel(experts, *refs),
        out_shape=shapes,
        in_specs=[pl.BlockSpec(memory_space=pltpu.SMEM)]
        + [pl.BlockSpec(memory_space=pltpu.HBM)] * 4,
        scratch_shapes=[pltpu.VMEM(a.shape, a.dtype) for a in operands]
        + [pltpu.SemaphoreType.DMA((4,))],
        cost_estimate=pl.CostEstimate(
            flops=3_000_000_000, transcendentals=0, bytes_accessed=4_000_000
        ),
        compiler_params=pltpu.CompilerParams(vmem_limit_bytes=SMALL_VMEM),
    )(base.reshape(1), *operands)


def experts_kernel(count, *refs):
    x_refs = refs[:count]
    gate_ref, up_ref, down_ref, keep_ref, give_ref = refs[count:]
    inner = gate_ref.shape[1]
    width = down_ref.shape[1]
    order = list(range(1, count, 2)) + list(range(0, count, 2))
    x = jnp.concatenate([x_refs[n][...] for n in order], axis=0)
    half = x.shape[0] // 2

    def product(a, b):
        return jnp.dot(a, b, preferred_element_type=jnp.float32)

    hidden = []
    for edge in range(0, inner, 256):
        cols = pl.ds(edge, min(256, inner - edge))
        gate, up = product(x, gate_ref[:, cols]), product(x, up_ref[:, cols])
        hidden.append((gate / (1.0 + jnp.exp(-gate)) * up).astype(jnp.bfloat16))
    hidden = jnp.concatenate(hidden, axis=1)
    for edge in range(0, width, width // 2):
        cols = pl.ds(edge, width // 2)
        part = product(hidden, down_ref[:, cols]).astype(jnp.bfloat16)
        shape = (*give_ref.shape[:2], width // 2)
        give_ref[:, :, cols] = part[:half].reshape(shape)
        keep_ref[:, :, cols] = part[half:].reshape(shape)


def expert_rows(pieces, weights):
    rows, width = pieces[0].shape
    inner = weights[0].shape[1]
    count = len(pieces)
    on_chip = pl.BlockSpec(memory_space=pltpu.VMEM)
    out = jax.ShapeDtypeStruct((count // 2, rows, width), jnp.bfloat16)
    return pl.pallas_call(
        lambda *refs: experts_kernel(count, *refs),
        out_shape=(out, out),
        in_specs=[on_chip] * (count + 3),
        cost_estimate=pl.CostEstimate(
            flops=6 * count * rows * width * inner,
            transcendentals=count * rows * inner,
            bytes_accessed=6 * width * inner,
        ),
        compiler_params=pltpu.CompilerParams(vmem_limit_bytes=EXPERT_VMEM),
    )(*pieces, *weights)


def small_call(kernel, out_shape):
    def call(*operands):
        return pl.pallas_call(
            kernel,
            out_shape=out_shape,
            cost_estimate=pl.CostEstimate(
                flops=1_000_000_000, transcendentals=0, bytes_accessed=1_000_000
            ),
            compiler_params=pltpu.CompilerParams(vmem_limit_bytes=SMALL_VMEM),
        )(*operands)

    return call


def pair_kernel(*refs):
    *blocks, out_ref = refs
    half = blocks[0].shape[1]
    rows = blocks[0].shape[0] // 2
    for side in range(2):
        parts = [ref[side * rows : (side + 1) * rows, :] for ref in blocks]
        out_ref[:, side * half : (side + 1) * half] = jnp.concatenate(parts, axis=0)


def pair(blocks):
    tall, half = blocks[0].shape
    shape = jax.ShapeDtypeStruct((len(blocks) * tall // 2, 2 * half), jnp.bfloat16)
    return small_call(pair_kernel, shape)(*blocks)


def fold_kernel(count, *refs):
    terms, outs = refs[: len(refs) - count], refs[len(refs) - count :]
    rows, half = outs[0].shape[0] // 2, outs[0].shape[1]
    for side in range(2):
        cols = slice(side * half, (side + 1) * half)
        values = [ref[0, :, cols] if len(ref.shape) == 3 else ref[:, cols] for ref in terms]
        summed = sum(value.astype(jnp.float32) for value in values).astype(jnp.bfloat16)
        for n, out_ref in enumerate(outs):
            out_ref[side * rows : (side + 1) * rows, :] = summed[n * rows : (n + 1) * rows]


def fold(terms, count):
    rows, width = terms[0].shape[-2:]
    shape = jax.ShapeDtypeStruct((2 * rows // count, width // 2), jnp.bfloat16)
    return small_call(functools.partial(fold_kernel, count), [shape] * count)(*terms)


def join_kernel(*refs):
    *pieces, out_ref = refs
    start = 0
    for piece in pieces:
        out_ref[start : start + piece.shape[0], :] = piece[...]
        start += piece.shape[0]


def join(pieces):
    count = sum(piece.shape[0] for piece in pieces)
    shape = jax.ShapeDtypeStruct((count, pieces[0].shape[1]), jnp.bfloat16)
    return small_call(join_kernel, shape)(*pieces)


def blend_kernel(keys, started, mix_ref, *refs):
    out_ref = refs[-1]
    rows = mix_ref.shape[2]
    sides = refs[0].shape[0] // rows
    half = refs[0].shape[1]
    for side in range(sides):
        cols = slice(side * half, (side + 1) * half)
        result = refs[-2][:, cols] if started else 0.0
        for key, rows_ref in zip(keys, refs):
            for n in range(2):
                result = result + lax.dot_general(
                    mix_ref[n, key],
                    rows_ref[side * rows : (side + 1) * rows, :],
                    (((0,), (0,)), ((), ())),
                    preferred_element_type=jnp.float32,
                )
        out_ref[:, cols] = result.astype(out_ref.dtype)


def blend(mix, rows, started, final):
    keys = sorted(rows)
    width = rows[keys[0]].size // mix.shape[2]
    operands = [rows[key] for key in keys] + ([] if started is None else [started])
    return pl.pallas_call(
        lambda *refs: blend_kernel(keys, started is not None, *refs),
        out_shape=jax.ShapeDtypeStruct(
            (mix.shape[3], width), jnp.bfloat16 if final else jnp.float32
        ),
        cost_estimate=pl.CostEstimate(
            flops=1_500_000_000, transcendentals=0, bytes_accessed=2_000_000
        ),
        compiler_params=pltpu.CompilerParams(vmem_limit_bytes=SMALL_VMEM),
    )(mix, *operands)


def attend_kernel(scaling, place_ref, q_ref, near_ref, far_ref, spots_ref, mix_ref, gain_ref, w_ref, *outs):
    keep_ref, give_ref = outs
    count = 2 * keep_ref.shape[0]
    rows = keep_ref.shape[1]
    value_dim = gain_ref.shape[1]
    key_dim = near_ref.shape[1] - value_dim
    heads = q_ref.shape[1]
    length = near_ref.shape[0]
    span = length
    while span > 2048 and span % 2 == 0:
        span = span // 2
    order = list(range(1, count, 2)) + list(range(0, count, 2))
    queries, spots = [], []
    for n in order:
        start = (place_ref[1] ^ n) * rows
        queries.append([q_ref[pl.ds(start, rows), head, :] for head in range(heads)])
        spots.append(place_ref[0] + start + lax.broadcasted_iota(jnp.int32, (rows, 1), 0))
    queries = [jnp.concatenate(part, axis=0) for part in zip(*queries)]
    spot = jnp.concatenate(spots, axis=0)
    lane = lax.broadcasted_iota(jnp.int32, (count * rows, key_dim), 1)
    attended = []
    for head in range(heads):
        mapped = []
        for m in range(2):
            chosen = (lane >= m * key_dim // 2) & (lane < (m + 1) * key_dim // 2)
            one = jnp.where(chosen, queries[head], 0.0)
            one = one.astype(jnp.bfloat16)

            def step(n, running, kv_ref, offset, one=one):
                peak, sums, numer = running
                here = pl.ds(n * span, span)
                there = pl.ds(offset + n * span, span)
                scores = lax.dot_general(
                    one,
                    kv_ref[here, :key_dim],
                    (((1,), (1,)), ((), ())),
                    preferred_element_type=jnp.float32,
                )
                visible = spots_ref[:, there] <= spot
                scores = jnp.where(visible, scores * scaling, NEG_LARGE)
                top = jnp.maximum(peak, jnp.max(scores, axis=1, keepdims=True))
                weights = jnp.exp(scores - top)
                factor = jnp.exp(peak - top)
                sums = sums * factor + jnp.sum(weights, axis=1, keepdims=True)
                numer = numer * factor + jnp.dot(
                    weights.astype(jnp.bfloat16),
                    kv_ref[here, key_dim:],
                    preferred_element_type=jnp.float32,
                )
                return top, sums, numer

            state = (
                jnp.full((count * rows, 1), NEG_LARGE, jnp.float32),
                jnp.zeros((count * rows, 1), jnp.float32),
                jnp.zeros((count * rows, value_dim), jnp.float32),
            )
            for kv_ref, offset in ((near_ref, 0), (far_ref, length)):
                if span == length:
                    state = step(0, state, kv_ref, offset)
                else:
                    state = lax.fori_loop(
                        0,
                        length // span,
                        functools.partial(step, kv_ref=kv_ref, offset=offset),
                        state,
                    )
            mapped.append(state[2] / state[1])
        blended = mapped[0] - mix_ref[head] * mapped[1]
        scale = lax.rsqrt(jnp.mean(blended * blended, axis=-1, keepdims=True) + 1e-05)
        attended.append((blended * scale * gain_ref[...]).astype(jnp.bfloat16))
    flat = jnp.concatenate(attended, axis=1)
    part = jnp.dot(flat, w_ref[...], preferred_element_type=jnp.float32).astype(jnp.bfloat16)
    give_ref[...] = part[: count // 2 * rows].reshape(give_ref.shape)
    keep_ref[...] = part[count // 2 * rows :].reshape(keep_ref.shape)


def attend(place, queries, both, spots, mix_scale, head_gain, out_weight, parts, scaling):
    rows_here = queries.shape[0]
    width = out_weight.shape[1]
    out = jax.ShapeDtypeStruct((parts // 2, rows_here // parts, width), jnp.bfloat16)
    small = pl.BlockSpec(memory_space=pltpu.SMEM)
    large = pl.BlockSpec(memory_space=pltpu.VMEM)
    return pl.pallas_call(
        lambda *refs: attend_kernel(scaling, *refs),
        out_shape=(out, out),
        in_specs=[small, large, large, large, large, small, large, large],
        cost_estimate=pl.CostEstimate(
            flops=5_000_000_000, transcendentals=0, bytes_accessed=4_000_000
        ),
        compiler_params=pltpu.CompilerParams(vmem_limit_bytes=VMEM_LIMIT),
    )(place, queries, *both, spots, mix_scale, head_gain.reshape(1, -1), out_weight)


def step(
    queries,
    keys,
    values,
    mix_scale,
    head_gain,
    out_weight,
    moe_input,
    norm_gain,
    routes,
    route_weights,
    gate_weight,
    up_weight,
    down_weight,
):
    rows_here, _, key_dim = queries.shape
    ep_size = lax.axis_size("ep")
    tp_size = lax.axis_size("tp")
    ep_index = lax.axis_index("ep").astype(jnp.int32)
    tp_index = lax.axis_index("tp").astype(jnp.int32)
    tok_count, width = moe_input.shape
    top_count = routes.shape[1]
    experts = ep_size * gate_weight.shape[0]
    capacity = max(2, 3 * top_count * tok_count // (2 * experts))
    split = ep_size <= 8

    both = jnp.concatenate([keys, values], axis=2).reshape(rows_here, -1)
    bits = bits_of("ep")
    held = [both]
    for bit in bits[:-1]:
        held.append(swap(both, "ep", bit))
        both = join(held)
        held = [both]
    both = [both, upward(both, "ep", bits[-1])]

    base = ep_index if split else jnp.zeros_like(ep_index)
    *blocks, mix = route_tokens(
        base, moe_input, norm_gain, routes, route_weights, experts, capacity, split
    )

    weights = [gate_weight[0], up_weight[0], down_weight[0]]
    if split:
        weights = [pltpu.with_memory_space_constraint(w, pltpu.VMEM) for w in weights]

    def expert_group(piece):
        pieces = spread(piece, "tp")
        keep, give = expert_rows(pieces, weights)
        return gather_sum(keep, give, "tp")

    if split:
        arrived = [blocks[0]] + [swap(blocks[k], "ep", k) for k in range(1, ep_size)]
        returned = {}
        for low in range(0, ep_size, 2):
            members = range(low, min(low + 2, ep_size))
            group = pair([arrived[k] for k in members])
            done = fold(expert_group(group), len(members))
            for k, block in zip(members, done):
                returned[k] = swap(block, "ep", k) if k else block
        early = {k: returned[k] for k in range(ep_size - 2)}
        late = {k: returned[k] for k in range(ep_size - 2, ep_size)}
        mixed = blend(mix, early, None, False)
        mixed = blend(mix, late, mixed, True)
    else:
        count = blocks[0].shape[0]

        def exchange(rows):
            rows = rows.reshape(ep_size, -1, width)
            rows = lax.all_to_all(rows, "ep", split_axis=0, concat_axis=0, tiled=True)
            return rows.reshape(count, width)

        back = exchange(total(first_rows(expert_group(exchange(blocks[0])))))
        mixed = blend(mix.reshape(2, 1, count, tok_count), {0: back}, None, True)

    place = jnp.stack([ep_index * rows_here, tp_index])
    length = 2 * both[0].shape[0]
    spots = jnp.arange(length, dtype=jnp.int32)
    spots = ((spots // rows_here) ^ ep_index) * rows_here + spots % rows_here
    keep, give = attend(
        place,
        queries,
        both,
        spots.reshape(1, -1),
        mix_scale,
        head_gain,
        out_weight.reshape(-1, width),
        tp_size,
        1.0 / math.sqrt(key_dim // 2),
    )
    terms = gather_sum(keep, give, "tp")
    attn_out = total(first_rows(terms))
    return attn_out, mixed


def solution(mesh):
    in_specs = (
        P("ep", "tp", None),
        P("ep", "tp", None),
        P("ep", "tp", None),
        P("tp"),
        P(),
        P("tp", None, None),
        P(("ep", "tp"), None),
        P(),
        P(("ep", "tp"), None),
        P(("ep", "tp"), None),
        P("ep", None, "tp"),
        P("ep", None, "tp"),
        P("ep", "tp", None),
    )
    out_specs = (P(("ep", "tp"), None), P(("ep", "tp"), None))
    return jax.shard_map(step, mesh=mesh, in_specs=in_specs, out_specs=out_specs, check_vma=False)
```

```python
import functools
import math

import jax
import jax.numpy as jnp
from jax import lax
from jax.experimental import pallas as pl
from jax.experimental.pallas import tpu as pltpu
from jax.sharding import PartitionSpec as P

NEG_LARGE = -1e30
VMEM_LIMIT = 40 * 1024 * 1024


def grant(arrays, factor, base=2):
    size = sum(a.size * jnp.dtype(a.dtype).itemsize for a in arrays)
    limit = base * 2**20 + factor * size
    return pltpu.CompilerParams(vmem_limit_bytes=min(limit, VMEM_LIMIT))


def swap(array, axis, bits):
    pairs = [(j, j ^ bits) for j in range(lax.axis_size(axis))]
    return lax.ppermute(array, axis, pairs)


def upward(array, axis, bit):
    pairs = [(j, j ^ bit) for j in range(lax.axis_size(axis)) if not j & bit]
    return lax.ppermute(array, axis, pairs)


def bits_of(axis):
    size = lax.axis_size(axis)
    return [1 << n for n in range(size.bit_length() - 1)]


def spread(piece, axis):
    bits = bits_of(axis)
    pieces = {0: piece}
    for bit in reversed(bits):
        for key in sorted(pieces):
            pieces[key | bit] = swap(pieces[key], axis, bit)
    return [pieces[key] for key in range(1 << len(bits))]


def total(terms):
    return sum(term.astype(jnp.float32) for term in terms).astype(jnp.bfloat16)


def gather_sum(keep, give, axis):
    bits = bits_of(axis)
    got = swap(give, axis, bits[0])
    parts = {2 * n: [keep[n], got[n]] for n in range(keep.shape[0])}
    for bit in bits[1:]:
        keys = [key for key in parts if not key & bit]
        if len(keys) == 1:
            sums = [total(parts[key | bit]) for key in keys]
            sent = [swap(one, axis, bit) for one in sums]
        else:
            sent = jnp.stack([total(parts[key | bit]) for key in keys])
            sent = swap(sent, axis, bit)
        parts = {key: parts[key] + [sent[n]] for n, key in enumerate(keys)}
    return [keep, got] + parts[0][2:]


def first_rows(terms):
    return [term[0] if term.ndim == 3 else term for term in terms]


def tokens_kernel(experts, base_ref, *refs):
    sources, outs = refs[:4], refs[4:-5]
    x_ref, gain_ref, routes_ref, shares_ref = refs[-5:-1]
    *blocks, table_ref = outs
    loads = [
        pltpu.make_async_copy(source, target, refs[-1].at[n])
        for n, (source, target) in enumerate(zip(sources, refs[-5:-1]))
    ]
    for load in loads:
        load.start()
    for load in loads:
        load.wait()
    tok_count = x_ref.shape[0]
    rows = blocks[0].size // (experts // len(blocks) * x_ref.shape[1])
    wide = x_ref[...].astype(jnp.float32)
    normed = wide * lax.rsqrt(jnp.mean(wide * wide, axis=-1, keepdims=True) + 1e-06)
    normed = (normed * gain_ref[...]).astype(jnp.bfloat16)
    routes, shares = routes_ref[...], shares_ref[...]
    expert = lax.broadcasted_iota(jnp.int32, (experts, tok_count), 0) ^ base_ref[0]
    named = jnp.zeros((experts, tok_count), jnp.float32)
    share = jnp.zeros((experts, tok_count), jnp.float32)
    for k in range(routes.shape[0]):
        hit = routes[k : k + 1, :] == expert
        named = named + jnp.where(hit, 1.0, 0.0)
        share = share + jnp.where(hit, shares[k : k + 1, :], 0.0)
    row = lax.broadcasted_iota(jnp.int32, (tok_count, tok_count), 0)
    col = lax.broadcasted_iota(jnp.int32, (tok_count, tok_count), 1)
    earlier = jnp.where(row < col, 1.0, 0.0).astype(jnp.bfloat16)
    ranks = jnp.dot(named.astype(jnp.bfloat16), earlier, preferred_element_type=jnp.float32)
    places = jnp.where(named > 0.5, ranks, -1.0)
    slot = lax.broadcasted_iota(jnp.int32, (rows, tok_count), 0).astype(jnp.float32)
    picks = [jnp.where(places[k : k + 1, :] == slot, 1.0, 0.0) for k in range(experts)]
    pick = jnp.concatenate(picks, axis=0).astype(jnp.bfloat16)
    sent = jnp.dot(pick, normed, preferred_element_type=jnp.float32).astype(jnp.bfloat16)
    if len(blocks) == 1:
        blocks[0][...] = sent
    else:
        half = sent.shape[1] // 2
        for k in range(experts):
            for side in range(2):
                part = sent[k * rows : (k + 1) * rows, side * half : (side + 1) * half]
                blocks[k][side * rows : (side + 1) * rows, :] = part
    table_ref[0] = places
    table_ref[1] = share


def route_tokens(base, moe_input, norm_gain, routes, route_weights, experts, capacity, split):
    tok_count, width = moe_input.shape
    operands = [moe_input, norm_gain.reshape(1, -1), routes.T, route_weights.T]
    operands = [pltpu.with_memory_space_constraint(a, pltpu.HBM) for a in operands]
    unit = 4 if split else 8
    rows = -(-capacity // unit) * unit
    if split:
        shapes = [jax.ShapeDtypeStruct((2 * rows, width // 2), jnp.bfloat16)] * experts
    else:
        shapes = [jax.ShapeDtypeStruct((experts * rows, width), jnp.bfloat16)]
    shapes.append(jax.ShapeDtypeStruct((2, experts, tok_count), jnp.float32))
    return pl.pallas_call(
        lambda *refs: tokens_kernel(experts, *refs),
        out_shape=shapes,
        in_specs=[pl.BlockSpec(memory_space=pltpu.SMEM)]
        + [pl.BlockSpec(memory_space=pltpu.HBM)] * 4,
        scratch_shapes=[pltpu.VMEM(a.shape, a.dtype) for a in operands]
        + [pltpu.SemaphoreType.DMA((4,))],
        cost_estimate=pl.CostEstimate(
            flops=3_000_000_000, transcendentals=0, bytes_accessed=4_000_000
        ),
        compiler_params=grant([*operands, *shapes], 3),
    )(base.reshape(1), *operands)


def experts_kernel(count, *refs):
    x_refs = refs[:count]
    gate_ref, up_ref, down_ref, keep_ref, give_ref = refs[count:]
    inner = gate_ref.shape[1]
    width = down_ref.shape[1]
    order = list(range(1, count, 2)) + list(range(0, count, 2))
    x = jnp.concatenate([x_refs[n][...] for n in order], axis=0)
    half = x.shape[0] // 2

    def product(a, b):
        return jnp.dot(a, b, preferred_element_type=jnp.float32)

    hidden = []
    for edge in range(0, inner, 256):
        cols = pl.ds(edge, min(256, inner - edge))
        gate, up = product(x, gate_ref[:, cols]), product(x, up_ref[:, cols])
        hidden.append((gate / (1.0 + jnp.exp(-gate)) * up).astype(jnp.bfloat16))
    hidden = jnp.concatenate(hidden, axis=1)
    for edge in range(0, width, width // 2):
        cols = pl.ds(edge, width // 2)
        part = product(hidden, down_ref[:, cols]).astype(jnp.bfloat16)
        shape = (*give_ref.shape[:2], width // 2)
        give_ref[:, :, cols] = part[:half].reshape(shape)
        keep_ref[:, :, cols] = part[half:].reshape(shape)


def expert_rows(pieces, weights, resident):
    rows, width = pieces[0].shape
    inner = weights[0].shape[1]
    count = len(pieces)
    on_chip = pl.BlockSpec(memory_space=pltpu.VMEM)
    out = jax.ShapeDtypeStruct((count // 2, rows, width), jnp.bfloat16)
    return pl.pallas_call(
        lambda *refs: experts_kernel(count, *refs),
        out_shape=(out, out),
        in_specs=[on_chip] * (count + 3),
        cost_estimate=pl.CostEstimate(
            flops=6 * count * rows * width * inner,
            transcendentals=count * rows * inner,
            bytes_accessed=6 * width * inner,
        ),
        compiler_params=grant([*pieces, out, out, *([] if resident else weights)], 2),
    )(*pieces, *weights)


def small_call(kernel, out_shape):
    def call(*operands):
        return pl.pallas_call(
            kernel,
            out_shape=out_shape,
            cost_estimate=pl.CostEstimate(
                flops=1_000_000_000, transcendentals=0, bytes_accessed=1_000_000
            ),
            compiler_params=grant(operands, 2),
        )(*operands)

    return call


def pair_kernel(*refs):
    *blocks, out_ref = refs
    half = blocks[0].shape[1]
    rows = blocks[0].shape[0] // 2
    for side in range(2):
        parts = [ref[side * rows : (side + 1) * rows, :] for ref in blocks]
        out_ref[:, side * half : (side + 1) * half] = jnp.concatenate(parts, axis=0)


def pair(blocks):
    tall, half = blocks[0].shape
    shape = jax.ShapeDtypeStruct((len(blocks) * tall // 2, 2 * half), jnp.bfloat16)
    return small_call(pair_kernel, shape)(*blocks)


def fold_kernel(count, *refs):
    terms, outs = refs[: len(refs) - count], refs[len(refs) - count :]
    rows, half = outs[0].shape[0] // 2, outs[0].shape[1]
    for side in range(2):
        cols = slice(side * half, (side + 1) * half)
        values = [ref[0, :, cols] if len(ref.shape) == 3 else ref[:, cols] for ref in terms]
        summed = sum(value.astype(jnp.float32) for value in values).astype(jnp.bfloat16)
        for n, out_ref in enumerate(outs):
            out_ref[side * rows : (side + 1) * rows, :] = summed[n * rows : (n + 1) * rows]


def fold(terms, count):
    rows, width = terms[0].shape[-2:]
    shape = jax.ShapeDtypeStruct((2 * rows // count, width // 2), jnp.bfloat16)
    return small_call(functools.partial(fold_kernel, count), [shape] * count)(*terms)


def join_kernel(*refs):
    *pieces, out_ref = refs
    start = 0
    for piece in pieces:
        out_ref[start : start + piece.shape[0], :] = piece[...]
        start += piece.shape[0]


def join(pieces):
    count = sum(piece.shape[0] for piece in pieces)
    shape = jax.ShapeDtypeStruct((count, pieces[0].shape[1]), jnp.bfloat16)
    return small_call(join_kernel, shape)(*pieces)


def blend_kernel(keys, count, started, table_ref, *refs):
    out_ref = refs[-1]
    tok_count, width = out_ref.shape
    rows = refs[0].size // (count * width)
    half = refs[0].shape[1]
    slot = lax.broadcasted_iota(jnp.int32, (rows, tok_count), 0).astype(jnp.float32)
    mixes = []
    for key in keys:
        parts = [
            jnp.where(table_ref[0, k : k + 1, :] == slot, table_ref[1, k : k + 1, :], 0.0)
            for k in range(key, key + count)
        ]
        mix = jnp.concatenate(parts, axis=0) if count > 1 else parts[0]
        high = mix.astype(jnp.bfloat16)
        mixes.append((high, (mix - high.astype(jnp.float32)).astype(jnp.bfloat16)))
    for side in range(width // half):
        cols = slice(side * half, (side + 1) * half)
        result = refs[-2][:, cols] if started else 0.0
        for pair_of, rows_ref in zip(mixes, refs):
            here = rows_ref[side * count * rows : (side + 1) * count * rows, :]
            for mix in pair_of:
                result = result + lax.dot_general(
                    mix, here, (((0,), (0,)), ((), ())), preferred_element_type=jnp.float32
                )
        out_ref[:, cols] = result.astype(out_ref.dtype)


def blend(table, rows, count, started, shape, final):
    keys = sorted(rows)
    operands = [rows[key] for key in keys] + ([] if started is None else [started])
    return pl.pallas_call(
        lambda *refs: blend_kernel(keys, count, started is not None, *refs),
        out_shape=jax.ShapeDtypeStruct(shape, jnp.bfloat16 if final else jnp.float32),
        cost_estimate=pl.CostEstimate(
            flops=1_500_000_000, transcendentals=0, bytes_accessed=2_000_000
        ),
        compiler_params=grant([table, *operands], 2, 3),
    )(table, *operands)


def attend_kernel(scaling, place_ref, q_ref, near_ref, far_ref, spots_ref, mix_ref, gain_ref, w_ref, *outs):
    keep_ref, give_ref = outs
    count = 2 * keep_ref.shape[0]
    rows = keep_ref.shape[1]
    value_dim = gain_ref.shape[1]
    key_dim = near_ref.shape[1] - value_dim
    heads = q_ref.shape[1]
    length = near_ref.shape[0]
    span = length
    while span > 2048 and span % 2 == 0:
        span = span // 2
    order = list(range(1, count, 2)) + list(range(0, count, 2))
    queries, spots = [], []
    for n in order:
        start = (place_ref[1] ^ n) * rows
        queries.append([q_ref[pl.ds(start, rows), head, :] for head in range(heads)])
        spots.append(place_ref[0] + start + lax.broadcasted_iota(jnp.int32, (rows, 1), 0))
    queries = [jnp.concatenate(part, axis=0) for part in zip(*queries)]
    spot = jnp.concatenate(spots, axis=0)
    lane = lax.broadcasted_iota(jnp.int32, (count * rows, key_dim), 1)
    attended = []
    for head in range(heads):
        mapped = []
        for m in range(2):
            chosen = (lane >= m * key_dim // 2) & (lane < (m + 1) * key_dim // 2)
            one = jnp.where(chosen, queries[head], 0.0)
            one = one.astype(jnp.bfloat16)

            def step(n, running, kv_ref, offset, one=one):
                peak, sums, numer = running
                here = pl.ds(n * span, span)
                there = pl.ds(offset + n * span, span)
                scores = lax.dot_general(
                    one,
                    kv_ref[here, :key_dim],
                    (((1,), (1,)), ((), ())),
                    preferred_element_type=jnp.float32,
                )
                visible = spots_ref[:, there] <= spot
                scores = jnp.where(visible, scores * scaling, NEG_LARGE)
                top = jnp.maximum(peak, jnp.max(scores, axis=1, keepdims=True))
                weights = jnp.exp(scores - top)
                factor = jnp.exp(peak - top)
                sums = sums * factor + jnp.sum(weights, axis=1, keepdims=True)
                numer = numer * factor + jnp.dot(
                    weights.astype(jnp.bfloat16),
                    kv_ref[here, key_dim:],
                    preferred_element_type=jnp.float32,
                )
                return top, sums, numer

            state = (
                jnp.full((count * rows, 1), NEG_LARGE, jnp.float32),
                jnp.zeros((count * rows, 1), jnp.float32),
                jnp.zeros((count * rows, value_dim), jnp.float32),
            )
            for kv_ref, offset in ((near_ref, 0), (far_ref, length)):
                if span == length:
                    state = step(0, state, kv_ref, offset)
                else:
                    state = lax.fori_loop(
                        0,
                        length // span,
                        functools.partial(step, kv_ref=kv_ref, offset=offset),
                        state,
                    )
            mapped.append(state[2] / state[1])
        blended = mapped[0] - mix_ref[head] * mapped[1]
        scale = lax.rsqrt(jnp.mean(blended * blended, axis=-1, keepdims=True) + 1e-05)
        attended.append((blended * scale * gain_ref[...]).astype(jnp.bfloat16))
    flat = jnp.concatenate(attended, axis=1)
    part = jnp.dot(flat, w_ref[...], preferred_element_type=jnp.float32).astype(jnp.bfloat16)
    give_ref[...] = part[: count // 2 * rows].reshape(give_ref.shape)
    keep_ref[...] = part[count // 2 * rows :].reshape(keep_ref.shape)


def attend(place, queries, both, spots, mix_scale, head_gain, out_weight, parts, scaling):
    rows_here = queries.shape[0]
    width = out_weight.shape[1]
    out = jax.ShapeDtypeStruct((parts // 2, rows_here // parts, width), jnp.bfloat16)
    small = pl.BlockSpec(memory_space=pltpu.SMEM)
    large = pl.BlockSpec(memory_space=pltpu.VMEM)
    return pl.pallas_call(
        lambda *refs: attend_kernel(scaling, *refs),
        out_shape=(out, out),
        in_specs=[small, large, large, large, large, small, large, large],
        cost_estimate=pl.CostEstimate(
            flops=5_000_000_000, transcendentals=0, bytes_accessed=4_000_000
        ),
        compiler_params=grant([queries, out_weight, out, out, *both], 2, 8),
    )(place, queries, *both, spots, mix_scale, head_gain.reshape(1, -1), out_weight)


def step(
    queries,
    keys,
    values,
    mix_scale,
    head_gain,
    out_weight,
    moe_input,
    norm_gain,
    routes,
    route_weights,
    gate_weight,
    up_weight,
    down_weight,
):
    rows_here, _, key_dim = queries.shape
    ep_size = lax.axis_size("ep")
    tp_size = lax.axis_size("tp")
    ep_index = lax.axis_index("ep").astype(jnp.int32)
    tp_index = lax.axis_index("tp").astype(jnp.int32)
    tok_count, width = moe_input.shape
    top_count = routes.shape[1]
    experts = ep_size * gate_weight.shape[0]
    capacity = max(2, 3 * top_count * tok_count // (2 * experts))
    split = ep_size <= 8

    both = jnp.concatenate([keys, values], axis=2).reshape(rows_here, -1)
    bits = bits_of("ep")
    held = [both]
    for bit in bits[:-1]:
        held.append(swap(both, "ep", bit))
        both = join(held)
        held = [both]
    both = [both, upward(both, "ep", bits[-1])]

    base = ep_index if split else jnp.zeros_like(ep_index)
    *blocks, table = route_tokens(
        base, moe_input, norm_gain, routes, route_weights, experts, capacity, split
    )

    weights = [gate_weight[0], up_weight[0], down_weight[0]]
    if split:
        weights = [pltpu.with_memory_space_constraint(w, pltpu.VMEM) for w in weights]

    def expert_group(piece):
        pieces = spread(piece, "tp")
        keep, give = expert_rows(pieces, weights, split)
        return gather_sum(keep, give, "tp")

    if split:
        arrived = [blocks[0]] + [swap(blocks[k], "ep", k) for k in range(1, ep_size)]
        returned = {}
        for low in range(0, ep_size, 2):
            members = range(low, min(low + 2, ep_size))
            group = pair([arrived[k] for k in members])
            done = fold(expert_group(group), len(members))
            for k, block in zip(members, done):
                returned[k] = swap(block, "ep", k) if k else block
        early = {k: returned[k] for k in range(ep_size - 2)}
        late = {k: returned[k] for k in range(ep_size - 2, ep_size)}
        shape = moe_input.shape
        mixed = blend(table, early, 1, None, shape, False)
        mixed = blend(table, late, 1, mixed, shape, True)
    else:
        count = blocks[0].shape[0]

        def exchange(rows):
            rows = rows.reshape(ep_size, -1, width)
            rows = lax.all_to_all(rows, "ep", split_axis=0, concat_axis=0, tiled=True)
            return rows.reshape(count, width)

        back = exchange(total(first_rows(expert_group(exchange(blocks[0])))))
        mixed = blend(table, {0: back}, experts, None, moe_input.shape, True)

    place = jnp.stack([ep_index * rows_here, tp_index])
    length = 2 * both[0].shape[0]
    spots = jnp.arange(length, dtype=jnp.int32)
    spots = ((spots // rows_here) ^ ep_index) * rows_here + spots % rows_here
    keep, give = attend(
        place,
        queries,
        both,
        spots.reshape(1, -1),
        mix_scale,
        head_gain,
        out_weight.reshape(-1, width),
        tp_size,
        1.0 / math.sqrt(key_dim // 2),
    )
    terms = gather_sum(keep, give, "tp")
    attn_out = total(first_rows(terms))
    return attn_out, mixed


def solution(mesh):
    in_specs = (
        P("ep", "tp", None),
        P("ep", "tp", None),
        P("ep", "tp", None),
        P("tp"),
        P(),
        P("tp", None, None),
        P(("ep", "tp"), None),
        P(),
        P(("ep", "tp"), None),
        P(("ep", "tp"), None),
        P("ep", None, "tp"),
        P("ep", None, "tp"),
        P("ep", "tp", None),
    )
    out_specs = (P(("ep", "tp"), None), P(("ep", "tp"), None))
    return jax.shard_map(step, mesh=mesh, in_specs=in_specs, out_specs=out_specs, check_vma=False)
```
